32 devices in a mesh: sp: 8 (over z, x), tp: 4 (over y, core).
Axes of the slice: x: 2, y: 2, z: 4, core: 2. Of those that a mesh axis runs over, the one named last changes fastest.
Arguments:
- stream: bfloat16 [4096, 2048], P(('sp', 'tp')), may hold values from -6 to 6
- pool_in: bfloat16 [4096, 1024], P('sp', 'tp'), may hold values from -6 to 6
- doc_ids: int32 [4096], P('sp'), may hold values from 0 to 7, never falling along the last dimension, each value on 1 to 1024 neighbouring positions
- pool_map: bfloat16 [4, 256, 512], P('tp'), may hold values from -0.375 to 0.375
- pool_scale: float32 [2048], P('tp'), may hold values from 0.1 to 1.9
- out_weight: bfloat16 [2048, 2048], P('tp'), may hold values from -0.125 to 0.125
- norm_gain: float32 [2048], replicated, may hold values from 0.1 to 1.9
- routes: int32 [4096, 2], P('sp'), may hold values from 0 to 7, all different within a row; in each aligned block of 128 rows (0 to 127, 128 to 255, ...) at most 48 rows name the same one
- route_weight: float32 [4096, 2], P(('sp', 'tp')), may hold values from 0.2 to 1
- expert_gate: bfloat16 [8, 2048, 1024], P('sp', None, 'tp'), may hold values from -0.125 to 0.125
- expert_up: bfloat16 [8, 2048, 1024], P('sp', None, 'tp'), may hold values from -0.125 to 0.125
- expert_down: bfloat16 [8, 1024, 2048], P('sp', 'tp'), may hold values from -0.1875 to 0.1875
Outputs:
- result: bfloat16 [4096, 2048], P(('sp', 'tp'))
The draws below stay inside these ranges and needn't reach their ends.
Inputs may be any that keep to these rules, and one draw needn't show every extreme that they name: `routes`: each token names 2 different experts; in each aligned block of 128 rows no expert is named by more than 48 rows, a bound that some block reaches. `doc_ids`: never falling; each document holds at most 1024 positions.
All inputs are finite; a program needn't handle non-finite values.
Results may differ from the reference program's by a relative error of at most 0.014.
Values may be sent and summed in bfloat16 or wider, within the bound.
A program may use at most 64 MiB of HBM per device.

```python
import math
import jax
import jax.numpy as jnp
import numpy as np
from jax import lax

D = 2048
PW = 1024
GROUPS = 4
FF = 1024
TOPK = 2
DOC_COUNT = 8
GW = 256
GOUT = 512
QUART = 128
TOKENS = 4096
EXPERTS = 8
CAP = 48
FF_PART = 256
DOC_MOST = 1024
N_TP = 4


def block_levels(rng, dims, cuts, low, high):
    loudness, own = 1.0, jax.random.fold_in(rng, 6)
    for dim, blocks in cuts:
        heights = jnp.exp(jax.random.uniform(jax.random.fold_in(own, dim), (blocks,), jnp.float32, low / len(cuts), high / len(cuts)))
        loudness = loudness * jnp.repeat(heights, dims[dim] // blocks).reshape([-1 if axis == dim else 1 for axis in range(len(dims))])
    return loudness


def split_up(number_of, total, bound, lean):
    loads = [(1 << 20) // math.isqrt(rank ** lean) + 1 for rank in range(2, number_of + 1)]
    spare, holding = total - bound - (number_of - 1), [1] * (number_of - 1)
    while spare > 0:
        candidates = [i for i in range(number_of - 1) if holding[i] < bound]
        pool, budget = sum([loads[i] for i in candidates]), spare
        for i in candidates:
            addition = min(bound - holding[i], max(1, budget * loads[i] // pool), spare)
            holding[i] = holding[i] + addition
            spare = spare - addition
    return np.array([bound] + holding)


def ragged_sizes(stream_key, number_of, total, reach, lean):
    if number_of == 2:
        one = jax.random.randint(stream_key, (), max(1, total - reach), min(reach, total - 1) + 1)
        return jnp.stack([one, total - one])
    lengths = jnp.asarray(split_up(number_of, total, reach, lean), jnp.int32)
    twos = (number_of - 1) // 2
    donor, receiver = lengths[1:1 + 2 * twos:2], lengths[2:2 + 2 * twos:2]
    slack = jnp.minimum(donor - 1, reach - receiver)
    passed = jax.random.randint(jax.random.fold_in(stream_key, 1), (twos,), 0, 1 << 20) % (slack + 1)
    lengths = lengths.at[1:1 + 2 * twos:2].set(donor - passed).at[2:2 + 2 * twos:2].set(receiver + passed)
    return lengths[jax.random.permutation(jax.random.fold_in(stream_key, 2), number_of)]


def routed_block(rng, own, number, rows, number_of, top, most, skew):
    order = jax.random.permutation(rng, number_of)
    heavy_load, usual = shares(number_of, rows * top, most, skew, True), shares(number_of, rows * top, most, skew, False)
    places = jnp.arange(number_of)

    def named(tallies, rotation):
        used = int((tallies > 0).sum())
        fixed = max(1, used // 4)
        moved = fixed + (places - fixed + rotation * (used - fixed)) % max(1, number_of - fixed)
        return jnp.zeros((number_of,), jnp.int32).at[order[jnp.where(places < fixed, places, moved)]].set(jnp.asarray(tallies, jnp.int32))

    tallies = jnp.where(number % 4 == 0, named(heavy_load, number // 4), named(usual, number - number // 4 - 1))
    mixed = jax.random.permutation(jax.random.fold_in(own, 3), number_of)
    giver, sink = mixed[0:number_of // 2 * 2:2], mixed[1:number_of // 2 * 2:2]
    margin = jnp.minimum(tallies[giver] - 1, most - tallies[sink]) // 2
    margin = jnp.where((giver == order[0]) | (sink == order[0]) | (tallies[sink] == 0), 0, jnp.maximum(margin, 0))
    moved = jax.random.randint(jax.random.fold_in(own, 4), (number_of // 2,), 0, 1 << 20) % (margin + 1)
    tallies = tallies.at[giver].add(-moved).at[sink].add(moved)
    items = jnp.searchsorted(jnp.cumsum(tallies), jnp.arange(rows * top), side="right").astype(jnp.int32)
    grid = items.reshape(top, rows).T
    grid = grid[jax.random.permutation(jax.random.fold_in(own, 1), rows)]
    rotation = jax.random.randint(jax.random.fold_in(own, 2), (rows, 1), 0, top)
    return jnp.take_along_axis(grid, (jnp.arange(top)[None, :] + rotation) % top, axis=1)


def shares(number_of, total, bound, skew, full):
    portions = [(1 << 20) // math.isqrt(grade ** skew) + 1 for grade in range(1, number_of + 1)]
    largest = bound if full else min(bound, max(-(-total // number_of), total * portions[0] // sum(portions)))
    least = 1 if total - largest >= number_of - 1 else 0
    given, rest = [largest] + [least] * (number_of - 1), total - largest - least * (number_of - 1)
    while rest > 0:
        movable = [i for i in range(1, number_of) if given[i] < largest] or [i for i in range(1, number_of) if given[i] < bound]
        whole, left = sum([portions[i] for i in movable]), rest
        for i in movable:
            more = min(bound - given[i], max(1, left * portions[i] // whole), rest)
            given[i] = given[i] + more
            rest = rest - more
    return np.array(given)


def normal_values(stream_key, shape, width, limit, pieces=(), kind=jnp.bfloat16):
    drawn = width * jax.random.normal(stream_key, shape, jnp.float32)
    if pieces:
        drawn = drawn * block_levels(stream_key, shape, pieces, -0.22, 0.18)
    return jnp.clip(drawn, -limit, limit).astype(kind)


def setup_inputs(seed: int = 0) -> dict:
    streams_of = jax.random.split(jax.random.key(seed), 13)
    stream = normal_values(streams_of[0], (TOKENS, D), 1.0, 6.0, ((0, 32),))
    pool_in = normal_values(streams_of[1], (TOKENS, PW), 1.0, 6.0, ((0, 8), (1, 4)))
    doc_ids = jnp.searchsorted(jnp.cumsum(ragged_sizes(streams_of[2], DOC_COUNT, TOKENS, DOC_MOST, 1)), jnp.arange(TOKENS), side="right").astype(jnp.int32)
    pool_map = normal_values(streams_of[3], (GROUPS, GW, GOUT), GW ** -0.5, 0.375, ((0, 4),))
    pool_scale = jnp.clip(1.0 + 0.18 * jax.random.normal(streams_of[4], (D,), jnp.float32), 0.1, 1.9)
    out_weight = normal_values(streams_of[5], (D, D), D ** -0.5, 0.125, ((0, 4),))
    norm_gain = jnp.clip(1.0 + 0.18 * jax.random.normal(streams_of[6], (D,), jnp.float32), 0.1, 1.9)
    routes_keys = jax.random.split(jax.random.fold_in(streams_of[7], 1), TOKENS // QUART)
    routes_turns = jax.random.permutation(jax.random.fold_in(streams_of[7], 3), TOKENS // QUART)
    routes = jax.vmap(lambda own, number: routed_block(jax.random.fold_in(streams_of[7], 2), own, number, QUART, EXPERTS, TOPK, CAP, 1))(routes_keys, routes_turns).reshape((TOKENS, TOPK))
    route_weight = jnp.clip(0.2 + 0.8 * jax.random.uniform(streams_of[8], (TOKENS, TOPK), jnp.float32) ** block_levels(streams_of[8], (TOKENS, TOPK), ((0, 32),), -0.2, 0.2), 0.2, 1.0)
    expert_gate = normal_values(streams_of[9], (EXPERTS, D, FF), D ** -0.5, 0.125, ((0, 8), (2, 4)))
    expert_up = normal_values(streams_of[10], (EXPERTS, D, FF), D ** -0.5, 0.125, ((0, 8), (2, 4)))
    expert_down = normal_values(streams_of[11], (EXPERTS, FF, D), FF ** -0.5, 0.1875, ((0, 8), (1, 4)))
    return dict(stream=stream, pool_in=pool_in, doc_ids=doc_ids, pool_map=pool_map, pool_scale=pool_scale, out_weight=out_weight, norm_gain=norm_gain, routes=routes, route_weight=route_weight, expert_gate=expert_gate, expert_up=expert_up, expert_down=expert_down)


EPS = 1e-06

def reference(stream, pool_in, doc_ids, pool_map, pool_scale, out_weight, norm_gain, routes, route_weight, expert_gate, expert_up, expert_down):
    total_rows = pool_in.shape[0]
    positions = jnp.arange(total_rows, dtype=jnp.int32)
    starts_here = jnp.concatenate([jnp.ones((1,), jnp.bool_), doc_ids[1:] != doc_ids[:-1]])
    doc_start = lax.cummax(jnp.where(starts_here, positions, 0).astype(jnp.int32), axis=0)
    source_rows = pool_in.astype(jnp.float32)
    branch_parts = []
    for group_index in range(GROUPS):
        window = 2 << group_index
        group_cols = source_rows[:, group_index * GW:(group_index + 1) * GW]
        running = jnp.zeros_like(group_cols)
        counts = jnp.zeros((total_rows,), jnp.float32)
        for offset in range(window):
            shifted = jnp.concatenate([jnp.zeros((offset, GW), jnp.float32), group_cols[:total_rows - offset]], axis=0)
            in_window = positions - offset >= doc_start
            running = running + jnp.where(in_window[:, None], shifted, 0.0)
            counts = counts + in_window.astype(jnp.float32)
        pooled = (running / counts[:, None] - group_cols).astype(jnp.bfloat16)
        mapped = jnp.dot(pooled, pool_map[group_index], preferred_element_type=jnp.float32)
        branch_parts.append((mapped * pool_scale[group_index * GOUT:(group_index + 1) * GOUT]).astype(jnp.bfloat16))
    branch = jnp.concatenate(branch_parts, axis=1)
    mixed_rows = (stream.astype(jnp.float32) + jnp.dot(branch, out_weight, preferred_element_type=jnp.float32)).astype(jnp.bfloat16)
    mixed_up = mixed_rows.astype(jnp.float32)
    normed = (mixed_up * lax.rsqrt(lax.optimization_barrier(jnp.mean(mixed_up * mixed_up, axis=1, keepdims=True)) + EPS) * norm_gain).astype(jnp.bfloat16)
    block_count = total_rows // QUART
    flattened = routes.reshape(-1).astype(jnp.int32)
    one_hot = (flattened[:, None] == jnp.arange(EXPERTS, dtype=jnp.int32)[None, :]).astype(jnp.int32)
    blocked = one_hot.reshape(block_count, QUART * TOPK, EXPERTS)
    ranking = lax.optimization_barrier(jnp.sum((jnp.cumsum(blocked, axis=1) - blocked) * blocked, axis=2)).reshape(-1).astype(jnp.int32)
    assign_ids = jnp.arange(total_rows * TOPK, dtype=jnp.int32)
    block_ids = (assign_ids // (QUART * TOPK)).astype(jnp.int32)
    target_slot = ((flattened * block_count + block_ids) * CAP + ranking).astype(jnp.int32)
    per_expert = block_count * CAP
    slot_token = jnp.zeros((EXPERTS * per_expert,), jnp.int32).at[target_slot].set((assign_ids // TOPK).astype(jnp.int32))
    slot_weight = jnp.zeros((EXPERTS * per_expert,), jnp.float32).at[target_slot].set(route_weight.reshape(-1))

    def one_expert(accumulated, expert_index):
        begin_slot = (expert_index * per_expert).astype(jnp.int32)
        tokens_here = lax.dynamic_slice_in_dim(slot_token, begin_slot, per_expert)
        weights_here = lax.dynamic_slice_in_dim(slot_weight, begin_slot, per_expert)
        inputs = normed[tokens_here]
        gate_pre = jnp.dot(inputs, expert_gate[expert_index], preferred_element_type=jnp.float32)
        up_pre = jnp.dot(inputs, expert_up[expert_index], preferred_element_type=jnp.float32)
        hidden = (jax.nn.silu(gate_pre) * up_pre).astype(jnp.bfloat16)
        down_rows = expert_down[expert_index]
        summed = jnp.zeros((per_expert, D), jnp.float32)
        for part_index in range(N_TP):
            part_begin = part_index * FF_PART
            part_out = jnp.dot(hidden[:, part_begin:part_begin + FF_PART], down_rows[part_begin:part_begin + FF_PART], preferred_element_type=jnp.float32).astype(jnp.bfloat16)
            summed = summed + lax.optimization_barrier(part_out).astype(jnp.float32)
        expert_out = lax.optimization_barrier(summed.astype(jnp.bfloat16)).astype(jnp.float32)
        return (accumulated.at[tokens_here].add(weights_here[:, None] * expert_out), None)
    accumulated, unused_out = lax.scan(one_expert, jnp.zeros((total_rows, D), jnp.float32), jnp.arange(EXPERTS, dtype=jnp.int32))
    return (mixed_up + accumulated).astype(jnp.bfloat16)
```

```python
import functools

import jax
import jax.numpy as jnp
from jax import lax
from jax.experimental import pallas as pl
from jax.experimental.pallas import tpu as pltpu
from jax.sharding import PartitionSpec as P

HALO = 16
EPS = 1e-06
MESH = pl.DeviceIdType.MESH
F32 = jnp.float32
BF16 = jnp.bfloat16


def kernel(
    n_sp, n_tp, quarter, capacity, top,
    stream, pool_in, docs, pool_map, pool_scale, out_weight, gain, routes, weights,
    gate, up, down,
    out,
    gates, ups, downs, outw, halo, halo_docs, branch, pair_send, pair_recv, far_send, far_recv,
    mixed, dispatch, arrived, acc, answers, returned,
    local_sem, halo_ssem, halo_rsem, w_ssem, w_rsem, f_ssem, p_ssem, p_rsem,
    y_ssem, y_rsem, d_ssem, d_rsem, r_ssem, r_rsem,
):
    sp, tp = lax.axis_index("sp"), lax.axis_index("tp")
    n_chip = n_tp // 2
    chip, parity = tp // 2, tp % 2
    other = 1 - parity
    partner = chip * 2 + other
    rows = pool_in.shape[0]
    width = stream.shape[1]
    ff = gate.shape[1]
    slots = n_sp * capacity

    def same(m):
        return (chip + m) % n_chip * 2 + parity

    def remote(src, dst, ssem, rsem, to):
        return pltpu.make_async_remote_copy(
            src_ref=src, dst_ref=dst, send_sem=ssem, recv_sem=rsem,
            device_id=to, device_id_type=MESH,
        )

    half = width // 2
    pieces = (
        (gate.at[pl.ds(0, half)], lambda j: gates.at[j, pl.ds(0, half)]),
        (gate.at[pl.ds(half, half)], lambda j: gates.at[j, pl.ds(half, half)]),
        (up, lambda j: ups.at[j]),
        (down, lambda j: downs.at[j]),
    )
    count = len(pieces)

    own_copies = [
        pltpu.make_async_copy(out_weight, outw, local_sem.at[0]),
        pltpu.make_async_copy(gate, gates.at[0], local_sem.at[1]),
        pltpu.make_async_copy(up, ups.at[0], local_sem.at[2]),
        pltpu.make_async_copy(down, downs.at[0], local_sem.at[3]),
    ]
    for c in own_copies:
        c.start()

    barrier = pltpu.get_barrier_semaphore()
    for d in range(1, n_sp):
        pl.semaphore_signal(barrier, inc=1, device_id=((sp + d) % n_sp, tp), device_id_type=MESH)
    pl.semaphore_signal(barrier, inc=1, device_id=(sp, partner), device_id_type=MESH)
    for m in range(1, n_chip):
        pl.semaphore_signal(barrier, inc=1, device_id=(sp, same(m)), device_id_type=MESH)
    pl.semaphore_wait(barrier, n_sp - 1 + 1 + n_chip - 1)

    right = ((sp + 1) % n_sp, tp)
    halo_copies = [
        remote(pool_in.at[pl.ds(rows - HALO, HALO)], halo, halo_ssem.at[0], halo_rsem.at[0], right),
        remote(docs.at[pl.ds(rows - HALO, HALO)], halo_docs, halo_ssem.at[1], halo_rsem.at[1], right),
    ]
    for c in halo_copies:
        c.start()

    def far_weight(p, m):
        j = 2 * ((n_chip - m) % n_chip)
        return remote(pieces[p][0], pieces[p][1](j), w_ssem.at[m, p], w_rsem.at[j, p], (sp, same(m)))

    def near_weight(p):
        return remote(pieces[p][0], pieces[p][1](1), w_ssem.at[0, p], w_rsem.at[1, p], (sp, partner))

    def forward(p, m):
        ref = pieces[p][1](2 * m)
        return remote(ref, pieces[p][1](2 * m + 1), f_ssem.at[m, p], w_rsem.at[2 * m + 1, p], (sp, partner))

    for m in range(1, n_chip):
        far_weight(0, m).start()

    lanes = lax.broadcasted_iota(jnp.int32, (quarter, 128), 1)
    own_routes = routes[pl.ds(pl.multiple_of(tp * quarter, quarter), quarter), :]
    hots = [(own_routes[:, k : k + 1] == lanes).astype(F32) for k in range(top)]
    named = functools.reduce(lambda a, b: a + b, hots)
    below = (
        lax.broadcasted_iota(jnp.int32, (quarter, quarter), 0)
        > lax.broadcasted_iota(jnp.int32, (quarter, quarter), 1)
    ).astype(BF16)
    before = jnp.dot(below, named.astype(BF16), preferred_element_type=F32)
    slot_lanes = lax.broadcasted_iota(jnp.int32, (quarter, slots), 1)
    picks = []
    for k in range(top):
        rank = jnp.sum(hots[k] * before, axis=1, keepdims=True).astype(jnp.int32)
        picks.append((slot_lanes == own_routes[:, k : k + 1] * capacity + rank).astype(F32))
    spread = jnp.transpose(functools.reduce(lambda a, b: a + b, picks)).astype(BF16)
    picks = [p.astype(BF16) for p in picks]

    for c in halo_copies:
        c.wait_recv()
    first = sp == 0
    prior = jnp.where(first, 0.0, halo[...].astype(F32))
    prior_docs = jnp.where(first, -1, halo_docs[...])
    own = pool_in[...].astype(F32)
    group_width = own.shape[1]
    ext_docs = jnp.concatenate([prior_docs, docs[...]], axis=0)
    total = jnp.concatenate([prior, own], axis=0)
    counts = jnp.ones(ext_docs.shape, F32)
    window = jnp.left_shift(jnp.int32(2), tp)
    step = 1
    while step < HALO:
        keep = (pltpu.roll(ext_docs, step, 0) == ext_docs) & (step < window)
        counts = counts + jnp.where(keep, pltpu.roll(counts, step, 0), 0.0)
        keep_wide = jnp.concatenate([keep.astype(F32)] * (group_width // 128), axis=1) > 0.5
        total = total + jnp.where(keep_wide, pltpu.roll(total, step, 0), 0.0)
        step *= 2
    counts_wide = jnp.concatenate([counts] * (group_width // 128), axis=1)
    pooled = (total[HALO:] / counts_wide[HALO:] - own).astype(BF16)
    branch[...] = (
        jnp.dot(pooled, pool_map[...], preferred_element_type=F32) * pool_scale[...]
    ).astype(BF16)

    own_copies[0].wait()

    def share(owner):
        begin = pl.multiple_of(owner * quarter, quarter)
        return jnp.dot(branch[pl.ds(begin, quarter), :], outw[...], preferred_element_type=F32)

    pair_copies = []
    chips = list(range(1, n_chip)) + [0]
    for m in chips:
        pair_send[m] = share((chip + m) % n_chip * 2 + other).astype(BF16)
        c = remote(pair_send.at[m], pair_recv.at[m], p_ssem.at[m], p_rsem.at[m], (sp, partner))
        c.start()
        pair_copies.append(c)
    far_copies = []
    mine = None
    for m, c in zip(chips, pair_copies):
        block = share(same(m))
        c.wait_recv()
        block = block + pair_recv[m].astype(F32)
        if m == 0:
            mine = block
        else:
            far_send[m] = block.astype(BF16)
            j = (n_chip - m) % n_chip
            f = remote(far_send.at[m], far_recv.at[j], y_ssem.at[m], y_rsem.at[j], (sp, same(m)))
            f.start()
            far_copies.append(f)
            for p in range(1, count):
                far_weight(p, m).start()
    for p in range(count):
        near_weight(p).start()
    for m, f in zip(chips, far_copies):
        f.wait_recv()
        mine = mine + far_recv[(n_chip - m) % n_chip].astype(F32)
    mixed[...] = (stream[...].astype(F32) + mine).astype(BF16)
    value = mixed[...].astype(F32)
    normed = (
        value * lax.rsqrt(jnp.mean(value * value, axis=1, keepdims=True) + EPS) * gain[...]
    ).astype(BF16)

    dispatch[...] = jnp.dot(spread, normed, preferred_element_type=F32).astype(BF16)

    def part(ref, e):
        return ref.at[pl.ds(pl.multiple_of(e * capacity, 16), capacity)]

    def to_peer(src, dst, ssem, rsem, d):
        peer = (sp + d) % n_sp
        return remote(part(src, peer), part(dst, sp), ssem.at[d], rsem.at[d], (peer, tp))

    outward = [to_peer(dispatch, arrived, d_ssem, d_rsem, d) for d in range(1, n_sp)]
    for c in outward:
        c.start()
    mine_at = pl.ds(pl.multiple_of(sp * capacity, 16), capacity)
    arrived[mine_at, :] = dispatch[mine_at, :]

    for p in range(count - 1):
        for m in range(1, n_chip):
            remote(pieces[p][0], pieces[p][1](2 * m), w_ssem.at[m, p], w_rsem.at[2 * m, p], (sp, partner)).wait_recv()
            forward(p, m).start()
    for c in own_copies[1:]:
        c.wait()
    for c in outward:
        c.wait_recv()

    cols = 512

    def expert(j):
        x = arrived[...]
        g = jnp.dot(x, gates[j], preferred_element_type=F32)
        u = jnp.dot(x, ups[j], preferred_element_type=F32)
        return (g / (1.0 + jnp.exp(-g)) * u).astype(BF16)

    def project(j, hidden, begin):
        at = pl.ds(begin, cols)
        return jnp.dot(hidden, downs[j, :, at], preferred_element_type=F32).astype(BF16).astype(F32)

    for j in range(n_tp):
        if j % 2 == 1:
            for p in range(count - 1):
                remote(pieces[p][0], pieces[p][1](j), w_ssem.at[0, p], w_rsem.at[j, p], (sp, partner)).wait_recv()
        hidden = expert(j)
        p = count - 1
        if j >= 2 and j % 2 == 0:
            m = j // 2
            remote(pieces[p][0], pieces[p][1](j), w_ssem.at[m, p], w_rsem.at[j, p], (sp, partner)).wait_recv()
            forward(p, m).start()
        if j % 2 == 1:
            remote(pieces[p][0], pieces[p][1](j), w_ssem.at[0, p], w_rsem.at[j, p], (sp, partner)).wait_recv()
        for begin in range(0, width, cols):
            at = pl.ds(begin, cols)
            y = project(j, hidden, begin)
            if j == 0:
                acc[:, at] = y
            elif j < n_tp - 1:
                acc[:, at] += y
            else:
                answers[:, at] = (acc[:, at] + y).astype(BF16)

    back = [to_peer(answers, returned, r_ssem, r_rsem, d) for d in range(1, n_sp)]
    for c in back:
        c.start()
    returned[mine_at, :] = answers[mine_at, :]
    for c in back:
        c.wait_recv()
    for begin in range(0, width, cols):
        at = pl.ds(begin, cols)
        result = mixed[:, at].astype(F32)
        for k in range(top):
            result = result + weights[:, k : k + 1] * jnp.dot(
                picks[k], returned[:, at], preferred_element_type=F32
            )
        out[:, at] = result.astype(BF16)

    for c in halo_copies + pair_copies + far_copies + outward + back:
        c.wait_send()
    for p in range(count):
        near_weight(p).wait_send()
        for m in range(1, n_chip):
            far_weight(p, m).wait_send()
            forward(p, m).wait_send()


def per_device(
    n_sp, n_tp,
    stream, pool_in, doc_ids, pool_map, pool_scale, out_weight, norm_gain, routes, route_weight,
    expert_gate, expert_up, expert_down,
):
    rows, group_width = pool_in.shape
    quarter, width = stream.shape
    top = routes.shape[1]
    ff = expert_gate.shape[2]
    capacity = max(2, 3 * top * quarter // (2 * n_sp))
    capacity = -(-capacity // 16) * 16
    slots = n_sp * capacity
    n_chip = n_tp // 2
    vmem = pl.BlockSpec(memory_space=pltpu.VMEM)
    hbm = pl.BlockSpec(memory_space=pl.ANY)
    dma = pltpu.SemaphoreType.DMA
    V = pltpu.VMEM
    branch_width = out_weight.shape[0]
    return pl.pallas_call(
        functools.partial(kernel, n_sp, n_tp, quarter, capacity, top),
        out_shape=jax.ShapeDtypeStruct((quarter, width), BF16),
        in_specs=[vmem] * 5 + [hbm] + [vmem] * 3 + [hbm] * 3,
        out_specs=vmem,
        scratch_shapes=[
            V((n_tp, width, ff), BF16),
            V((n_tp, width, ff), BF16),
            V((n_tp, ff, width), BF16),
            V((branch_width, width), BF16),
            V((HALO, group_width), BF16),
            V((HALO, 128), jnp.int32),
            V((rows, branch_width), BF16),
            V((n_chip, quarter, width), BF16),
            V((n_chip, quarter, width), BF16),
            V((n_chip, quarter, width), BF16),
            V((n_chip, quarter, width), BF16),
            V((quarter, width), BF16),
            V((slots, width), BF16),
            V((slots, width), BF16),
            V((slots, width), F32),
            V((slots, width), BF16),
            V((slots, width), BF16),
            dma((4,)),
            dma((2,)),
            dma((2,)),
            dma((n_chip, 4)),
            dma((n_tp, 4)),
            dma((n_chip, 4)),
            dma((n_chip,)),
            dma((n_chip,)),
            dma((n_chip,)),
            dma((n_chip,)),
            dma((n_sp,)),
            dma((n_sp,)),
            dma((n_sp,)),
            dma((n_sp,)),
        ],
        compiler_params=pltpu.CompilerParams(
            collective_id=0, has_side_effects=True, vmem_limit_bytes=60 * 1024 * 1024
        ),
    )(
        stream, pool_in, jnp.broadcast_to(doc_ids[:, None], (rows, 128)), pool_map[0],
        pool_scale[None, :], out_weight, norm_gain[None, :], routes, route_weight,
        expert_gate[0], expert_up[0], expert_down[0],
    )


def solution(mesh):
    in_specs = (
        P(("sp", "tp"), None),
        P("sp", "tp"),
        P("sp"),
        P("tp", None, None),
        P("tp"),
        P("tp", None),
        P(),
        P("sp", None),
        P(("sp", "tp"), None),
        P("sp", None, "tp"),
        P("sp", None, "tp"),
        P("sp", "tp", None),
    )
    out_specs = P(("sp", "tp"), None)
    return jax.shard_map(
        functools.partial(per_device, mesh.shape["sp"], mesh.shape["tp"]),
        mesh=mesh, in_specs=in_specs, out_specs=out_specs, check_vma=False,
    )
```

```python
import functools

import jax
import jax.numpy as jnp
from jax import lax
from jax.experimental import pallas as pl
from jax.experimental.pallas import tpu as pltpu
from jax.sharding import PartitionSpec as P

HALO = 16
COLS = 512
EPS = 1e-06
MESH = pl.DeviceIdType.MESH
F32 = jnp.float32
BF16 = jnp.bfloat16


def kernel(
    n_sp, n_tp, quarter, capacity, top,
    stream, pool_in, docs_row, pool_map, pool_scale, out_weight, gain, routes, weights,
    gate, up, down,
    out,
    gates, ups, downs, outw, halo, halo_docs, branch, pair_send, pair_recv, far_send, far_recv,
    mixed, dispatch, arrived, hiddens, answers, returned, docs,
    local_sem, halo_ssem, halo_rsem, w_ssem, w_rsem, f_ssem, p_ssem, p_rsem,
    y_ssem, y_rsem, d_ssem, d_rsem, r_ssem, r_rsem,
):
    sp, tp = lax.axis_index("sp"), lax.axis_index("tp")
    n_chip = n_tp // 2
    chip, parity = tp // 2, tp % 2
    other = 1 - parity
    partner = chip * 2 + other
    rows = pool_in.shape[0]
    width = stream.shape[1]
    ff = gate.shape[1]
    slots = n_sp * capacity

    def same(m):
        return (chip + m) % n_chip * 2 + parity

    def remote(src, dst, ssem, rsem, to):
        return pltpu.make_async_remote_copy(
            src_ref=src, dst_ref=dst, send_sem=ssem, recv_sem=rsem,
            device_id=to, device_id_type=MESH,
        )

    half = width // 2
    pieces = (
        (gate.at[pl.ds(0, half)], lambda j: gates.at[j, pl.ds(0, half)]),
        (gate.at[pl.ds(half, half)], lambda j: gates.at[j, pl.ds(half, half)]),
        (up, lambda j: ups.at[j]),
    ) + tuple(
        (
            down.at[:, pl.ds(begin, COLS)],
            lambda j, begin=begin: downs.at[j, :, pl.ds(begin, COLS)],
        )
        for begin in range(0, width, COLS)
    )
    count = len(pieces)
    early = 3

    own_copies = [
        pltpu.make_async_copy(out_weight, outw, local_sem.at[0]),
        pltpu.make_async_copy(gate, gates.at[0], local_sem.at[1]),
        pltpu.make_async_copy(up, ups.at[0], local_sem.at[2]),
        pltpu.make_async_copy(down, downs.at[0], local_sem.at[3]),
    ]
    for c in own_copies:
        c.start()

    barrier = pltpu.get_barrier_semaphore()
    for d in range(1, n_sp):
        pl.semaphore_signal(barrier, inc=1, device_id=((sp + d) % n_sp, tp), device_id_type=MESH)
    pl.semaphore_signal(barrier, inc=1, device_id=(sp, partner), device_id_type=MESH)
    for m in range(1, n_chip):
        pl.semaphore_signal(barrier, inc=1, device_id=(sp, same(m)), device_id_type=MESH)
    pl.semaphore_wait(barrier, n_sp - 1 + 1 + n_chip - 1)

    docs[...] = jnp.transpose(jnp.broadcast_to(docs_row[...].astype(F32), (128, rows)))
    right = ((sp + 1) % n_sp, tp)
    halo_copies = [
        remote(pool_in.at[pl.ds(rows - HALO, HALO)], halo, halo_ssem.at[0], halo_rsem.at[0], right),
        remote(docs.at[pl.ds(rows - HALO, HALO)], halo_docs, halo_ssem.at[1], halo_rsem.at[1], right),
    ]
    for c in halo_copies:
        c.start()

    def far_weight(p, m):
        j = 2 * ((n_chip - m) % n_chip)
        return remote(pieces[p][0], pieces[p][1](j), w_ssem.at[m, p], w_rsem.at[j, p], (sp, same(m)))

    def near_weight(p):
        return remote(pieces[p][0], pieces[p][1](1), w_ssem.at[0, p], w_rsem.at[1, p], (sp, partner))

    def forward(p, m):
        ref = pieces[p][1](2 * m)
        return remote(ref, pieces[p][1](2 * m + 1), f_ssem.at[m, p], w_rsem.at[2 * m + 1, p], (sp, partner))

    for m in range(1, n_chip):
        far_weight(0, m).start()

    names = lax.broadcasted_iota(jnp.int32, (128, quarter), 0)
    own_routes = routes[:, pl.ds(pl.multiple_of(tp * quarter, quarter), quarter)]
    hots = [(own_routes[k : k + 1, :] == names).astype(F32) for k in range(top)]
    named = functools.reduce(lambda a, b: a + b, hots)
    above = (
        lax.broadcasted_iota(jnp.int32, (quarter, quarter), 0)
        < lax.broadcasted_iota(jnp.int32, (quarter, quarter), 1)
    ).astype(BF16)
    before = jnp.dot(named.astype(BF16), above, preferred_element_type=F32)
    slot_names = lax.broadcasted_iota(jnp.int32, (slots, quarter), 0)
    places = []
    for k in range(top):
        rank = jnp.sum(hots[k] * before, axis=0, keepdims=True).astype(jnp.int32)
        places.append((slot_names == own_routes[k : k + 1, :] * capacity + rank).astype(F32))
    spread = functools.reduce(lambda a, b: a + b, places).astype(BF16)
    picks = [jnp.transpose(p).astype(BF16) for p in places]
    scales = [
        jnp.transpose(jnp.broadcast_to(weights[k : k + 1, :], (128, quarter)))[:, :1]
        for k in range(top)
    ]

    for c in halo_copies:
        c.wait_recv()
    first = sp == 0
    prior = jnp.where(first, 0.0, halo[...].astype(F32))
    prior_docs = jnp.where(first, -1.0, halo_docs[...])
    own = pool_in[...].astype(F32)
    group_width = own.shape[1]
    ext_docs = jnp.concatenate([prior_docs, docs[...]], axis=0)
    total = jnp.concatenate([prior, own], axis=0)
    counts = jnp.ones(ext_docs.shape, F32)
    window = jnp.left_shift(jnp.int32(2), tp)
    step = 1
    while step < HALO:
        keep = (pltpu.roll(ext_docs, step, 0) == ext_docs) & (step < window)
        counts = counts + jnp.where(keep, pltpu.roll(counts, step, 0), 0.0)
        keep_wide = jnp.concatenate([keep.astype(F32)] * (group_width // 128), axis=1) > 0.5
        total = total + jnp.where(keep_wide, pltpu.roll(total, step, 0), 0.0)
        step *= 2
    counts_wide = jnp.concatenate([counts] * (group_width // 128), axis=1)
    pooled = (total[HALO:] / counts_wide[HALO:] - own).astype(BF16)
    branch[...] = (
        jnp.dot(pooled, pool_map[...], preferred_element_type=F32) * pool_scale[...]
    ).astype(BF16)

    own_copies[0].wait()

    def share(owner):
        begin = pl.multiple_of(owner * quarter, quarter)
        return jnp.dot(branch[pl.ds(begin, quarter), :], outw[...], preferred_element_type=F32)

    pair_copies = []
    chips = list(range(1, n_chip)) + [0]
    for m in chips:
        pair_send[m] = share((chip + m) % n_chip * 2 + other).astype(BF16)
        c = remote(pair_send.at[m], pair_recv.at[m], p_ssem.at[m], p_rsem.at[m], (sp, partner))
        c.start()
        pair_copies.append(c)
    far_copies = []
    mine = None
    for m, c in zip(chips, pair_copies):
        block = share(same(m))
        c.wait_recv()
        block = block + pair_recv[m].astype(F32)
        if m == 0:
            mine = block
        else:
            far_send[m] = block.astype(BF16)
            j = (n_chip - m) % n_chip
            f = remote(far_send.at[m], far_recv.at[j], y_ssem.at[m], y_rsem.at[j], (sp, same(m)))
            f.start()
            far_copies.append(f)
            for p in range(1, count):
                far_weight(p, m).start()
    for p in range(count):
        near_weight(p).start()
    for m, f in zip(chips, far_copies):
        f.wait_recv()
        mine = mine + far_recv[(n_chip - m) % n_chip].astype(F32)
    mixed[...] = (stream[...].astype(F32) + mine).astype(BF16)
    value = mixed[...].astype(F32)
    normed = (
        value * lax.rsqrt(jnp.mean(value * value, axis=1, keepdims=True) + EPS) * gain[...]
    ).astype(BF16)

    dispatch[...] = jnp.dot(spread, normed, preferred_element_type=F32).astype(BF16)

    def part(ref, e, at):
        return ref.at[pl.ds(pl.multiple_of(e * capacity, 16), capacity), at]

    def to_peer(src, dst, ssem, rsem, d, at):
        peer = (sp + d) % n_sp
        return remote(part(src, peer, at), part(dst, sp, at), ssem, rsem, (peer, tp))

    everything = pl.ds(0, width)
    outward = [
        to_peer(dispatch, arrived, d_ssem.at[d], d_rsem.at[d], d, everything)
        for d in range(1, n_sp)
    ]
    for c in outward:
        c.start()
    mine_at = pl.ds(pl.multiple_of(sp * capacity, 16), capacity)
    arrived[mine_at, :] = dispatch[mine_at, :]

    def landed(p, j):
        remote(
            pieces[p][0], pieces[p][1](j), w_ssem.at[0, p], w_rsem.at[j, p], (sp, partner)
        ).wait_recv()

    for p in range(early):
        for m in range(1, n_chip):
            landed(p, 2 * m)
            forward(p, m).start()
    for c in own_copies[1:]:
        c.wait()
    for c in outward:
        c.wait_recv()

    for j in range(n_tp):
        if j % 2 == 1:
            for p in range(early):
                landed(p, j)
        x = arrived[...]
        g = jnp.dot(x, gates[j], preferred_element_type=F32)
        u = jnp.dot(x, ups[j], preferred_element_type=F32)
        hiddens[j] = (g / (1.0 + jnp.exp(-g)) * u).astype(BF16)

    back = []
    for p in range(early, count):
        at = pl.ds((p - early) * COLS, COLS)
        for m in range(1, n_chip):
            landed(p, 2 * m)
            forward(p, m).start()
        total = None
        for j in range(n_tp):
            if j % 2 == 1:
                landed(p, j)
            y = jnp.dot(hiddens[j], downs[j, :, at], preferred_element_type=F32)
            y = y.astype(BF16).astype(F32)
            total = y if total is None else total + y
        answers[:, at] = total.astype(BF16)
        for d in range(1, n_sp):
            c = to_peer(answers, returned, r_ssem.at[p - early, d], r_rsem.at[p - early, d], d, at)
            c.start()
            back.append(c)
        returned[mine_at, at] = answers[mine_at, at]

    for p in range(early, count):
        at = pl.ds((p - early) * COLS, COLS)
        for c in back[(p - early) * (n_sp - 1) : (p - early + 1) * (n_sp - 1)]:
            c.wait_recv()
        result = mixed[:, at].astype(F32)
        for k in range(top):
            result = result + scales[k] * jnp.dot(
                picks[k], returned[:, at], preferred_element_type=F32
            )
        out[:, at] = result.astype(BF16)

    for c in halo_copies + pair_copies + far_copies + outward + back:
        c.wait_send()
    for p in range(count):
        near_weight(p).wait_send()
        for m in range(1, n_chip):
            far_weight(p, m).wait_send()
            forward(p, m).wait_send()


def per_device(
    n_sp, n_tp,
    stream, pool_in, doc_ids, pool_map, pool_scale, out_weight, norm_gain, routes, route_weight,
    expert_gate, expert_up, expert_down,
):
    rows, group_width = pool_in.shape
    quarter, width = stream.shape
    top = routes.shape[1]
    ff = expert_gate.shape[2]
    capacity = max(2, 3 * top * quarter // (2 * n_sp))
    capacity = -(-capacity // 16) * 16
    slots = n_sp * capacity
    n_chip = n_tp // 2
    vmem = pl.BlockSpec(memory_space=pltpu.VMEM)
    hbm = pl.BlockSpec(memory_space=pl.ANY)
    dma = pltpu.SemaphoreType.DMA
    V = pltpu.VMEM
    branch_width = out_weight.shape[0]
    pieces = 3 + width // COLS
    return pl.pallas_call(
        functools.partial(kernel, n_sp, n_tp, quarter, capacity, top),
        out_shape=jax.ShapeDtypeStruct((quarter, width), BF16),
        in_specs=[vmem] * 5 + [hbm] + [vmem] * 3 + [hbm] * 3,
        out_specs=vmem,
        scratch_shapes=[
            V((n_tp, width, ff), BF16),
            V((n_tp, width, ff), BF16),
            V((n_tp, ff, width), BF16),
            V((branch_width, width), BF16),
            V((HALO, group_width), BF16),
            V((HALO, 128), F32),
            V((rows, branch_width), BF16),
            V((n_chip, quarter, width), BF16),
            V((n_chip, quarter, width), BF16),
            V((n_chip, quarter, width), BF16),
            V((n_chip, quarter, width), BF16),
            V((quarter, width), BF16),
            V((slots, width), BF16),
            V((slots, width), BF16),
            V((n_tp, slots, ff), BF16),
            V((slots, width), BF16),
            V((slots, width), BF16),
            V((rows, 128), F32),
            dma((4,)),
            dma((2,)),
            dma((2,)),
            dma((n_chip, pieces)),
            dma((n_tp, pieces)),
            dma((n_chip, pieces)),
            dma((n_chip,)),
            dma((n_chip,)),
            dma((n_chip,)),
            dma((n_chip,)),
            dma((n_sp,)),
            dma((n_sp,)),
            dma((width // COLS, n_sp)),
            dma((width // COLS, n_sp)),
        ],
        compiler_params=pltpu.CompilerParams(
            collective_id=0, has_side_effects=True, vmem_limit_bytes=60 * 1024 * 1024
        ),
    )(
        stream, pool_in, doc_ids[None, :], pool_map[0],
        pool_scale[None, :], out_weight, norm_gain[None, :], routes.T, route_weight.T,
        expert_gate[0], expert_up[0], expert_down[0],
    )


def solution(mesh):
    in_specs = (
        P(("sp", "tp"), None),
        P("sp", "tp"),
        P("sp"),
        P("tp", None, None),
        P("tp"),
        P("tp", None),
        P(),
        P("sp", None),
        P(("sp", "tp"), None),
        P("sp", None, "tp"),
        P("sp", None, "tp"),
        P("sp", "tp", None),
    )
    out_specs = P(("sp", "tp"), None)
    return jax.shard_map(
        functools.partial(per_device, mesh.shape["sp"], mesh.shape["tp"]),
        mesh=mesh, in_specs=in_specs, out_specs=out_specs, check_vma=False,
    )
```
